32 devices in a mesh: ep: 8 (over z, x), tp: 4 (over y, core).
Axes of the slice: x: 2, y: 2, z: 4, core: 2. Of those that a mesh axis runs over, the one named last changes fastest.
Arguments:
- tokens: bfloat16 [1536, 2048], P('ep'), may hold values from -6 to 6
- cotangent: bfloat16 [1536, 2048], P('ep'), may hold values from -6 to 6
- routing: int32 [1536, 2], P('ep'), may hold values from 0 to 7, all different within a row; in each aligned block of 192 rows (0 to 191, 192 to 383, ...) at most 60 rows name the same one
- route_weights: float32 [1536, 2], P('ep'), may hold values from 0.1 to 1
- w_gate: bfloat16 [8, 2048, 2048], P('ep', None, 'tp'), may hold values from -0.125 to 0.125
- w_up: bfloat16 [8, 2048, 2048], P('ep', None, 'tp'), may hold values from -0.125 to 0.125
- w_down: bfloat16 [8, 2048, 2048], P('ep', 'tp'), may hold values from -0.125 to 0.125
Outputs:
- grad_tokens: bfloat16 [1536, 2048], P('ep')
- grad_weights: bfloat16 [1536, 2], P('ep')
- grad_gate: bfloat16 [8, 2048, 2048], P('ep', None, 'tp')
- grad_up: bfloat16 [8, 2048, 2048], P('ep', None, 'tp')
- grad_down: bfloat16 [8, 2048, 2048], P('ep', 'tp')
The draws below stay inside these ranges and needn't reach their ends.
Inputs may be any that keep to these rules, and one draw needn't show every extreme that they name: `routing`: each row names 2 different experts. Within the rows of one device no expert is named more than 60 times, and in every draw some expert is named exactly 60 times by some device's rows.
All inputs are finite; a program needn't handle non-finite values.
Results may differ from the reference program's by a relative error of at most 0.019.
Values may be sent and summed in bfloat16 or wider, within the bound.
No kernel may reach another device: no remote copies, remote signals or barrier semaphores. Data moves between devices by JAX's collectives and lax.ppermute only.
A program may use at most 64 MiB of HBM per device.

```python
import math
import jax
import jax.numpy as jnp
import numpy as np
from jax import lax

D = 2048
F = 2048
TOP = 2
TOK_DEV = 192
EXPERTS = 8
CAP = 60
TOKENS = 1536
N_EP = 8
N_TP = 4


def levels(stream_key, dims, cuts, least, top_value):
    gain, own = 1.0, jax.random.fold_in(stream_key, 6)
    for axis_at, blocks in cuts:
        draws = jnp.exp(jax.random.uniform(jax.random.fold_in(own, axis_at), (blocks,), jnp.float32, least / len(cuts), top_value / len(cuts)))
        gain = gain * jnp.repeat(draws, dims[axis_at] // blocks).reshape([-1 if axis == axis_at else 1 for axis in range(len(dims))])
    return gain


def deal_out(key, own, number, rows, amount, top, most, lean):
    ranking = jax.random.permutation(key, amount)
    packed, ordinary = portions_of(amount, rows * top, most, lean, True), portions_of(amount, rows * top, most, lean, False)
    places = jnp.arange(amount)

    def named(lengths, turn):
        used = int((lengths > 0).sum())
        fixed = max(1, used // 4)
        shifted = fixed + (places - fixed + turn * (used - fixed)) % max(1, amount - fixed)
        return jnp.zeros((amount,), jnp.int32).at[ranking[jnp.where(places < fixed, places, shifted)]].set(jnp.asarray(lengths, jnp.int32))

    lengths = jnp.where(number % 4 == 0, named(packed, number // 4), named(ordinary, number - number // 4 - 1))
    mixed = jax.random.permutation(jax.random.fold_in(own, 3), amount)
    donor, sink = mixed[0:amount // 2 * 2:2], mixed[1:amount // 2 * 2:2]
    room = jnp.minimum(lengths[donor] - 1, most - lengths[sink]) // 2
    room = jnp.where((donor == ranking[0]) | (sink == ranking[0]) | (lengths[sink] == 0), 0, jnp.maximum(room, 0))
    shifted = jax.random.randint(jax.random.fold_in(own, 4), (amount // 2,), 0, 1 << 20) % (room + 1)
    lengths = lengths.at[donor].add(-shifted).at[sink].add(shifted)
    members = jnp.searchsorted(jnp.cumsum(lengths), jnp.arange(rows * top), side="right").astype(jnp.int32)
    grid = members.reshape(top, rows).T
    grid = grid[jax.random.permutation(jax.random.fold_in(own, 1), rows)]
    turn = jax.random.randint(jax.random.fold_in(own, 2), (rows, 1), 0, top)
    return jnp.take_along_axis(grid, (jnp.arange(top)[None, :] + turn) % top, axis=1)


def portions_of(count, total, most, lean, full):
    loads = [(1 << 20) // math.isqrt(grade ** lean) + 1 for grade in range(1, count + 1)]
    largest = most if full else min(most, max(-(-total // count), total * loads[0] // sum(loads)))
    least = 1 if total - largest >= count - 1 else 0
    holding, surplus = [largest] + [least] * (count - 1), total - largest - least * (count - 1)
    while surplus > 0:
        candidates = [i for i in range(1, count) if holding[i] < largest] or [i for i in range(1, count) if holding[i] < most]
        pool, remaining = sum([loads[i] for i in candidates]), surplus
        for i in candidates:
            more = min(most - holding[i], max(1, remaining * loads[i] // pool), surplus)
            holding[i] = holding[i] + more
            surplus = surplus - more
    return np.array(holding)


def noise(key, extent, spread, most, cuts=(), kind=jnp.bfloat16):
    factor_of = levels(key, extent, cuts, -0.22, 0.18) if cuts else 1.0
    drawn = jax.random.normal(key, extent, jnp.float32) * spread * factor_of
    return jnp.minimum(jnp.maximum(drawn, -most), most).astype(kind)


def setup_inputs(seed: int = 0) -> dict:
    keys = jax.random.split(jax.random.key(seed), 8)
    tokens = noise(keys[0], (TOKENS, D), 1.0, 6.0, ((0, 8),))
    cotangent = noise(keys[1], (TOKENS, D), 1.0, 6.0, ((0, 8),))
    routing_keys = jax.random.split(jax.random.fold_in(keys[2], 1), TOKENS // TOK_DEV)
    routing_turns = jax.random.permutation(jax.random.fold_in(keys[2], 3), TOKENS // TOK_DEV)
    routing = jax.vmap(lambda own, number: deal_out(jax.random.fold_in(keys[2], 2), own, number, TOK_DEV, EXPERTS, TOP, CAP, 2))(routing_keys, routing_turns).reshape((TOKENS, TOP))
    route_weights = jnp.clip(jnp.exp(math.log(1.0) - 2.3025851 * jax.random.uniform(keys[3], (TOKENS, TOP), jnp.float32) ** levels(keys[3], (TOKENS, TOP), ((0, 8),), -0.2, 0.2)), 0.1, 1.0)
    w_gate = noise(keys[4], (EXPERTS, D, F), D ** -0.5, 0.125, ((0, 8), (2, 4)))
    w_up = noise(keys[5], (EXPERTS, D, F), D ** -0.5, 0.125, ((0, 8), (2, 4)))
    w_down = noise(keys[6], (EXPERTS, F, D), F ** -0.5, 0.125, ((0, 8), (1, 4)))
    return {"tokens": tokens, "cotangent": cotangent, "routing": routing, "route_weights": route_weights, "w_gate": w_gate, "w_up": w_up, "w_down": w_down}


def reference(tokens, cotangent, routing, route_weights, w_gate, w_up, w_down):
    all_tokens = tokens.shape[0]
    experts = EXPERTS
    blocks = routing.reshape(N_EP, TOK_DEV * TOP)
    onehot = (blocks[:, :, None] == jnp.arange(experts, dtype=jnp.int32)[None, None, :]).astype(jnp.int32)
    before = jnp.cumsum(onehot, axis=1) - onehot
    within = jnp.sum(before * onehot, axis=2)
    source = jnp.arange(N_EP, dtype=jnp.int32)[:, None]
    place = (source * CAP + within).reshape(-1).astype(jnp.int32)
    expert_of = routing.reshape(-1).astype(jnp.int32)
    token_of = jnp.repeat(jnp.arange(all_tokens, dtype=jnp.int32), TOP)
    slot_count = N_EP * CAP
    table = jnp.full((experts, slot_count), all_tokens, jnp.int32).at[expert_of, place].set(token_of)
    rounded = lax.optimization_barrier(route_weights.astype(jnp.bfloat16)).astype(jnp.float32).reshape(-1)
    weight_table = jnp.zeros((experts, slot_count), jnp.float32).at[expert_of, place].set(rounded)
    padded_rows = jnp.concatenate([tokens, jnp.zeros((1, D), jnp.bfloat16)], 0)
    padded_back = jnp.concatenate([cotangent, jnp.zeros((1, D), jnp.bfloat16)], 0)
    hidden_block = F // N_TP

    def one_expert(args):
        index, weight, wgate, wup, wdown = args
        rows = padded_rows[index]
        back = padded_back[index]
        weight = weight[:, None]
        pre_gate = jnp.dot(rows, wgate, preferred_element_type=jnp.float32)
        pre_up = jnp.dot(rows, wup, preferred_element_type=jnp.float32)
        along = jnp.dot(back, wdown.T, preferred_element_type=jnp.float32)
        gate_sig = jax.nn.sigmoid(pre_gate)
        gate_act = pre_gate * gate_sig
        hidden = gate_act * pre_up
        hidden_grad = weight * along
        gate_grad = (hidden_grad * pre_up * gate_sig * (1.0 + pre_gate * (1.0 - gate_sig))).astype(jnp.bfloat16)
        up_grad = (hidden_grad * gate_act).astype(jnp.bfloat16)
        scaled = (weight * hidden).astype(jnp.bfloat16)
        grad_gate = jnp.dot(rows.T, gate_grad, preferred_element_type=jnp.float32).astype(jnp.bfloat16)
        grad_up = jnp.dot(rows.T, up_grad, preferred_element_type=jnp.float32).astype(jnp.bfloat16)
        grad_down = jnp.dot(scaled.T, back, preferred_element_type=jnp.float32).astype(jnp.bfloat16)
        slot_total = index.shape[0]
        gate_blocks = gate_grad.astype(jnp.float32).reshape(slot_total, N_TP, hidden_block)
        up_blocks = up_grad.astype(jnp.float32).reshape(slot_total, N_TP, hidden_block)
        wgate_blocks = wgate.astype(jnp.float32).reshape(D, N_TP, hidden_block)
        wup_blocks = wup.astype(jnp.float32).reshape(D, N_TP, hidden_block)
        row_part = jnp.einsum('rbf,dbf->rbd', gate_blocks, wgate_blocks) + jnp.einsum('rbf,dbf->rbd', up_blocks, wup_blocks)
        row_part = lax.optimization_barrier(row_part.astype(jnp.bfloat16)).astype(jnp.float32)
        slot_rows = jnp.sum(row_part, axis=1).astype(jnp.bfloat16)
        slot_part = jnp.sum((hidden * along).reshape(slot_total, N_TP, hidden_block), axis=2)
        slot_part = lax.optimization_barrier(slot_part.astype(jnp.bfloat16)).astype(jnp.float32)
        slot_grad = jnp.sum(slot_part, axis=1).astype(jnp.bfloat16)
        return slot_rows, slot_grad, grad_gate, grad_up, grad_down

    slot_rows, slot_grad, grad_gate, grad_up, grad_down = lax.map(
        one_expert, (table, weight_table, w_gate, w_up, w_down))
    picked = slot_rows[expert_of, place].astype(jnp.float32).reshape(all_tokens, TOP, D)
    grad_tokens = jnp.sum(picked, axis=1).astype(jnp.bfloat16)
    grad_weights = slot_grad[expert_of, place].reshape(all_tokens, TOP)
    return grad_tokens, grad_weights, grad_gate, grad_up, grad_down
```

```python
import jax
import jax.numpy as jnp
from jax import lax
from jax.sharding import PartitionSpec as P

BF = jnp.bfloat16
F32 = jnp.float32


def swap(x, mask):
    n = lax.axis_size("tp")
    return lax.ppermute(x, "tp", [(i, i ^ mask) for i in range(n)])


def gather_tp(block):
    n = lax.axis_size("tp")
    blocks = {0: block}
    mask = n // 2
    while mask:
        for d in list(blocks):
            blocks[d ^ mask] = swap(blocks[d], mask)
        mask //= 2
    return [blocks[d] for d in range(n)]


def reorder(x, mask):
    n = lax.axis_size("tp")
    rows = x.shape[0] // n
    return jnp.concatenate([x[(d ^ mask) * rows : ((d ^ mask) + 1) * rows] for d in range(n)], 0)


def on_device(tokens, cotangent, routing, route_weights, w_gate, w_up, w_down):
    experts = lax.axis_size("ep")
    n_tp = lax.axis_size("tp")
    me = lax.axis_index("tp")
    local_tokens, top_count = routing.shape
    width = tokens.shape[1]
    capacity = max(2, (5 * local_tokens * top_count + 4 * experts - 1) // (4 * experts))
    part = -(-capacity // n_tp)
    rows_q = part + 1
    if rows_q > 8:
        rows_q = -(-rows_q // 16) * 16
    spare = rows_q - 1
    block = experts * rows_q
    feat = width // n_tp

    flat = routing.reshape(-1)
    onehot = (flat[:, None] == jnp.arange(experts, dtype=jnp.int32)[None, :]).astype(jnp.int32)
    before = jnp.cumsum(onehot, axis=0) - onehot
    within = jnp.sum(before * onehot, axis=1)
    owner = within // part
    place = flat * rows_q + (within - owner * part)
    owner = owner.reshape(local_tokens, top_count)
    place = place.reshape(local_tokens, top_count)

    ids = jnp.arange(block, dtype=jnp.int32)[:, None, None]

    def picked_of(d):
        here = jnp.where(owner == (me ^ d), place, -1)
        return ids == here[None]

    mine = picked_of(0)
    by_token = jnp.any(mine, axis=2).astype(BF)
    slot_weight = jnp.sum(jnp.where(mine, route_weights[None], 0.0), axis=(1, 2))
    wrow = slot_weight.reshape(experts, rows_q)
    wrow = jnp.pad(wrow, ((0, 0), (0, width - rows_q)))[:, None, :]
    is_spare = (jnp.arange(rows_q) == spare)[None, :, None]
    send_rows = jnp.dot(by_token, tokens, preferred_element_type=F32).reshape(
        experts, rows_q, width
    )
    send_rows = jnp.where(is_spare, wrow, send_rows).astype(BF)
    send_back = jnp.dot(by_token, cotangent, preferred_element_type=F32).astype(BF)
    send_back = send_back.reshape(experts, rows_q, width)

    rows_in = lax.all_to_all(send_rows, "ep", split_axis=0, concat_axis=0, tiled=True)
    back_in = lax.all_to_all(send_back, "ep", split_axis=0, concat_axis=0, tiled=True)
    rows = jnp.concatenate(gather_tp(rows_in.reshape(block, width)), 0)
    back = jnp.concatenate(gather_tp(back_in.reshape(block, width)), 0)
    slots = n_tp * block
    weight = rows.reshape(n_tp * experts, rows_q, width)[:, spare, :rows_q]
    weight = weight.reshape(slots, 1).astype(F32)

    wgate = w_gate[0]
    wup = w_up[0]
    wdown = w_down[0]
    pre_gate = jnp.dot(rows, wgate, preferred_element_type=F32)
    pre_up = jnp.dot(rows, wup, preferred_element_type=F32)
    along = jnp.einsum("rd,fd->rf", back, wdown, preferred_element_type=F32)
    gate_sig = jax.nn.sigmoid(pre_gate)
    gate_act = pre_gate * gate_sig
    hidden = gate_act * pre_up
    hidden_grad = weight * along
    gate_grad = (hidden_grad * pre_up * gate_sig * (1.0 + pre_gate * (1.0 - gate_sig))).astype(BF)
    up_grad = (hidden_grad * gate_act).astype(BF)
    scaled = (weight * hidden).astype(BF)
    slot_part = jnp.sum(hidden * along, axis=1).astype(BF).astype(F32)
    srow = slot_part.reshape(n_tp * experts, rows_q)
    srow = jnp.pad(srow, ((0, 0), (0, feat - rows_q)))[:, None, :]

    def row_part(d):
        at = (me ^ d) * feat
        wg = lax.dynamic_slice_in_dim(wgate, at, feat, 0)
        wu = lax.dynamic_slice_in_dim(wup, at, feat, 0)
        out = jnp.einsum("rf,df->rd", gate_grad, wg, preferred_element_type=F32)
        out = out + jnp.einsum("rf,df->rd", up_grad, wu, preferred_element_type=F32)
        out = jnp.where(is_spare, srow, out.reshape(n_tp * experts, rows_q, feat))
        return out.astype(BF).reshape(slots, feat)

    order = sorted(range(n_tp), key=lambda d: -(d & 1) * n_tp - d)
    parts = {d: row_part(d) for d in order}
    mask = 1
    while mask < n_tp:
        for d in [d for d in sorted(parts, reverse=True) if d & mask]:
            got = reorder(swap(parts.pop(d), mask), mask)
            parts[d ^ mask] = (parts[d ^ mask].astype(F32) + got.astype(F32)).astype(BF)
        mask *= 2
    share = parts[0].reshape(n_tp, experts, rows_q, feat)
    home = lax.all_to_all(share, "ep", split_axis=1, concat_axis=1, tiled=True)

    grad_gate = jnp.einsum("rd,rf->df", rows, gate_grad, preferred_element_type=F32).astype(BF)
    grad_up = jnp.einsum("rd,rf->df", rows, up_grad, preferred_element_type=F32).astype(BF)
    grad_down = jnp.einsum("rf,rd->fd", scaled, back, preferred_element_type=F32).astype(BF)

    pick_home = jnp.concatenate([picked_of(d) for d in range(n_tp)], 0)
    home_by = jnp.any(pick_home, axis=2).astype(BF)
    feature_part = jnp.einsum(
        "st,sd->td", home_by, home.reshape(slots, feat), preferred_element_type=F32
    ).astype(BF)
    slot_grad = home[:, :, spare, :rows_q].reshape(slots, 1, 1).astype(F32)
    grad_weights = jnp.sum(jnp.where(pick_home, slot_grad, 0.0), axis=0).astype(BF)
    grad_tokens = lax.all_gather(feature_part, "tp", axis=1, tiled=True)
    return (grad_tokens, grad_weights, grad_gate[None], grad_up[None], grad_down[None])


def solution(mesh):
    row = P("ep", None)
    col = P("ep", None, "tp")
    low = P("ep", "tp", None)
    return jax.shard_map(
        on_device,
        mesh=mesh,
        in_specs=(row, row, row, row, col, col, low),
        out_specs=(row, row, col, col, low),
        check_vma=False,
    )
```

```python
import jax
import jax.numpy as jnp
from jax import lax
from jax.experimental import pallas as pl
from jax.experimental.pallas import tpu as pltpu
from jax.sharding import PartitionSpec as P

BF = jnp.bfloat16
F32 = jnp.float32


def swap(x, mask):
    n = lax.axis_size("tp")
    return lax.ppermute(x, "tp", [(i, i ^ mask) for i in range(n)])


def gather_tp(block, hold=None):
    n = lax.axis_size("tp")
    blocks = {0: block}
    mask = n // 2
    while mask:
        for d in list(blocks):
            sent = blocks[d]
            if hold is not None and mask == 1 and d in (0, n // 2):
                sent = hold(sent, d)
            blocks[d ^ mask] = swap(sent, mask)
        mask //= 2
    return [blocks[d] for d in range(n)]


def reorder(x, mask):
    n = lax.axis_size("tp")
    rows = x.shape[0] // n
    return jnp.concatenate([x[(d ^ mask) * rows : ((d ^ mask) + 1) * rows] for d in range(n)], 0)


def dispatch(me, routing, route_weights, tokens, cotangent, experts, part, rows_q):
    count, width = tokens.shape
    top_count = routing.shape[0]
    block = experts * rows_q

    def body(me_ref, route_ref, weight_ref, tok_ref, cot_ref, rows_ref, back_ref, within_ref):
        expert = lax.broadcasted_iota(jnp.int32, (experts, count), 0)
        names = [route_ref[k : k + 1, :] for k in range(top_count)]
        named = sum((name == expert).astype(F32) for name in names).astype(BF)
        earlier = lax.broadcasted_iota(jnp.int32, (count, count), 0) < lax.broadcasted_iota(
            jnp.int32, (count, count), 1
        )
        before = jnp.dot(named, earlier.astype(F32).astype(BF), preferred_element_type=F32)
        slot = lax.broadcasted_iota(jnp.int32, (block, count), 0)
        near = lax.broadcasted_iota(jnp.int32, (128, count), 0)
        picked = jnp.zeros((block, count), F32)
        spares = jnp.zeros((block, 128), F32)
        for k, name in enumerate(names):
            within = jnp.sum(jnp.where(name == expert, before, 0.0), axis=0, keepdims=True)
            within = within.astype(jnp.int32)
            within_ref[k : k + 1, :] = within
            local = within - me_ref[0] * part
            mine = (local >= 0) & (local < part)
            at = jnp.where(mine, name * rows_q + local, -1)
            picked = picked + (slot == at).astype(F32)
            row = jnp.where(mine, name * rows_q + rows_q - 1, -1)
            weight = jnp.where(near == local, weight_ref[k : k + 1, :], 0.0).astype(BF)
            spares = spares + lax.dot_general(
                (slot == row).astype(F32).astype(BF), weight, (((1,), (1,)), ((), ())),
                preferred_element_type=F32,
            )
        picked = picked.astype(BF)
        sent = jnp.dot(picked, tok_ref[...], preferred_element_type=F32)
        rows_ref[...] = sent.astype(BF)
        rows_ref[:, 0:128] = (sent[:, 0:128] + spares).astype(BF)
        sent = jnp.dot(picked, cot_ref[...], preferred_element_type=F32)
        back_ref[...] = sent.astype(BF)

    vmem = pl.BlockSpec(memory_space=pltpu.VMEM)
    return pl.pallas_call(
        body,
        name="dispatch",
        in_specs=[pl.BlockSpec(memory_space=pltpu.SMEM)] + [vmem] * 4,
        out_specs=[vmem] * 3,
        out_shape=[
            jax.ShapeDtypeStruct((block, width), BF),
            jax.ShapeDtypeStruct((block, width), BF),
            jax.ShapeDtypeStruct((top_count, count), jnp.int32),
        ],
    )(me.reshape(1).astype(jnp.int32), routing, route_weights, tokens, cotangent)


def on_device(tokens, cotangent, routing, route_weights, w_gate, w_up, w_down):
    experts = lax.axis_size("ep")
    n_tp = lax.axis_size("tp")
    me = lax.axis_index("tp")
    local_tokens, top_count = routing.shape
    width = tokens.shape[1]
    capacity = max(2, (5 * local_tokens * top_count + 4 * experts - 1) // (4 * experts))
    part = -(-capacity // n_tp)
    rows_q = part + 1
    if rows_q > 8:
        rows_q = -(-rows_q // 16) * 16
    spare = rows_q - 1
    block = experts * rows_q
    feat = width // n_tp

    routing = routing.T
    send_rows, send_back, within = dispatch(
        me, routing, route_weights.T, tokens, cotangent, experts, part, rows_q
    )
    send_rows = send_rows.reshape(experts, rows_q, width)
    send_back = send_back.reshape(experts, rows_q, width)
    is_spare = (jnp.arange(rows_q) == spare)[None, :, None]

    rows_in = lax.all_to_all(send_rows, "ep", split_axis=0, concat_axis=0, tiled=True)
    back_in = lax.all_to_all(send_back, "ep", split_axis=0, concat_axis=0, tiled=True)
    rows = jnp.concatenate(gather_tp(rows_in.reshape(block, width)), 0)
    wgate = w_gate[0]
    wup = w_up[0]
    wdown = w_down[0]
    pre_gate = jnp.dot(rows, wgate, preferred_element_type=F32)
    pre_up = jnp.dot(rows, wup, preferred_element_type=F32)

    def hold(blocks, d):
        nonlocal pre_gate, pre_up
        if d == 0:
            blocks, pre_gate = lax.optimization_barrier((blocks, pre_gate))
        else:
            blocks, pre_gate, pre_up = lax.optimization_barrier((blocks, pre_gate, pre_up))
        return blocks

    back = jnp.concatenate(gather_tp(back_in.reshape(block, width), hold), 0)
    slots = n_tp * block
    weight = rows.reshape(n_tp * experts, rows_q, width)[:, spare, :rows_q]
    weight = weight.reshape(slots, 1).astype(F32)

    along = jnp.einsum("rd,fd->rf", back, wdown, preferred_element_type=F32)
    gate_sig = jax.nn.sigmoid(pre_gate)
    gate_act = pre_gate * gate_sig
    hidden = gate_act * pre_up
    hidden_grad = weight * along
    gate_grad = (hidden_grad * pre_up * gate_sig * (1.0 + pre_gate * (1.0 - gate_sig))).astype(BF)
    up_grad = (hidden_grad * gate_act).astype(BF)
    scaled = (weight * hidden).astype(BF)
    slot_part = jnp.sum(hidden * along, axis=1).astype(BF).astype(F32)
    srow = slot_part.reshape(n_tp * experts, rows_q)
    srow = jnp.pad(srow, ((0, 0), (0, feat - rows_q)))[:, None, :]

    def row_part(d):
        at = (me ^ d) * feat
        wg = lax.dynamic_slice_in_dim(wgate, at, feat, 0)
        wu = lax.dynamic_slice_in_dim(wup, at, feat, 0)
        out = jnp.einsum("rf,df->rd", gate_grad, wg, preferred_element_type=F32)
        out = out + jnp.einsum("rf,df->rd", up_grad, wu, preferred_element_type=F32)
        out = jnp.where(is_spare, srow, out.reshape(n_tp * experts, rows_q, feat))
        return out.astype(BF).reshape(slots, feat)

    order = sorted(range(n_tp), key=lambda d: -(d & 1) * n_tp - d)
    parts = {d: row_part(d) for d in order}
    mask = 1
    while mask < n_tp:
        for d in [d for d in sorted(parts, reverse=True) if d & mask]:
            got = reorder(swap(parts.pop(d), mask), mask)
            parts[d ^ mask] = (parts[d ^ mask].astype(F32) + got.astype(F32)).astype(BF)
        mask *= 2
    share = parts[0].reshape(n_tp, experts, rows_q, feat)
    home = lax.all_to_all(share, "ep", split_axis=1, concat_axis=1, tiled=True)

    grad_gate = jnp.einsum("rd,rf->df", rows, gate_grad, preferred_element_type=F32).astype(BF)
    grad_up = jnp.einsum("rd,rf->df", rows, up_grad, preferred_element_type=F32).astype(BF)
    grad_down = jnp.einsum("rf,rd->fd", scaled, back, preferred_element_type=F32).astype(BF)

    owner = within // part
    within = within - owner * part
    at_block = (owner ^ me) * experts + routing
    ids = jnp.arange(slots, dtype=jnp.int32)[:, None]
    home_at = at_block * rows_q + within
    home_by = sum((ids == home_at[k : k + 1]).astype(BF) for k in range(top_count))
    feature_part = jnp.einsum(
        "st,sd->td", home_by, home.reshape(slots, feat), preferred_element_type=F32
    ).astype(BF)
    spares = home[:, :, spare, :rows_q].reshape(n_tp * experts, rows_q)
    pick_block = (jnp.arange(n_tp * experts)[:, None] == at_block.reshape(1, -1)).astype(BF)
    found = lax.dot_general(
        spares, pick_block, (((0,), (0,)), ((), ())), preferred_element_type=F32
    )
    lane = jnp.arange(rows_q)[:, None] == within.reshape(1, -1)
    grad_weights = jnp.sum(jnp.where(lane, found, 0.0), axis=0).astype(BF)
    grad_weights = grad_weights.reshape(top_count, local_tokens).T
    grad_tokens = lax.all_gather(feature_part, "tp", axis=1, tiled=True)
    return (grad_tokens, grad_weights, grad_gate[None], grad_up[None], grad_down[None])


def solution(mesh):
    row = P("ep", None)
    col = P("ep", None, "tp")
    low = P("ep", "tp", None)
    return jax.shard_map(
        on_device,
        mesh=mesh,
        in_specs=(row, row, row, row, col, col, low),
        out_specs=(row, row, col, col, low),
        check_vma=False,
    )
```
